32 devices in a mesh: sp: 16 (over z, y, x), tp: 2 (over core).
Axes of the slice: x: 2, y: 2, z: 4, core: 2. Of those that a mesh axis runs over, the one named last changes fastest.
Arguments:
- target: bfloat16 [4096, 1024], P(('sp', 'tp')), may hold values from -60 to 60
- source: bfloat16 [2048, 1024], P('sp'), may hold values from -7 to 7
- target_gains: bfloat16 [2, 4, 1024], replicated, may hold values from 0.099609375 to 1.8984375
- source_gain: bfloat16 [2, 1024], replicated, may hold values from 0.099609375 to 1.8984375
- query_weight: bfloat16 [2, 1024, 1024], P(None, None, 'tp'), may hold values from -0.1875 to 0.1875
- key_weight: bfloat16 [2, 1024, 1024], P(None, None, 'tp'), may hold values from -7.5625 to 7.5625
- value_weight: bfloat16 [2, 1024, 1024], P(None, None, 'tp'), may hold values from -0.1875 to 0.1875
- out_weight: bfloat16 [2, 1024, 1024], P(None, 'tp'), may hold values from -0.1875 to 0.1875
- gate_weight: bfloat16 [2, 1024, 1536], P(None, None, 'tp'), may hold values from -0.1875 to 0.1875
- up_weight: bfloat16 [2, 1024, 1536], P(None, None, 'tp'), may hold values from -0.1875 to 0.1875
- down_weight: bfloat16 [2, 1536, 1024], P(None, 'tp'), may hold values from -0.15625 to 0.15625
Outputs:
- stream: bfloat16 [4096, 1024], P(('sp', 'tp'))
The draws below stay inside these ranges and needn't reach their ends.
All inputs are finite; a program needn't handle non-finite values.
Results may differ from the reference program's by a relative error of at most 0.04.
Values may be sent and summed in bfloat16 or wider, within the bound.
No kernel may reach another device: no remote copies, remote signals or barrier semaphores. Data moves between devices by JAX's collectives and lax.ppermute only.
A program may use at most 64 MiB of HBM per device.

```python
import jax
import jax.numpy as jnp
from jax import lax

D = 1024
HEADS = 8
HEAD_DIM = 128
FF = 1536
LAYERS = 2
TGT_DEV = 256
TGT = 4096
SRC = 2048
N_TP = 2


def drawn_rows(key):
    base = jnp.clip(jax.random.normal(jax.random.fold_in(key, 101), (TGT, D), jnp.float32), -6.0, 6.0)
    return base


def draw_target(key, part):
    base = drawn_rows(key)
    return base.astype(jnp.bfloat16)


def draw_source(key, part):
    noise = jnp.clip(jax.random.normal(jax.random.fold_in(key, 105), (SRC, D), jnp.float32), -6.0, 6.0)
    return noise.astype(jnp.bfloat16)


def head_weights(key):
    shape = (LAYERS, D, HEADS * HEAD_DIM)
    first = jnp.clip(jax.random.normal(jax.random.fold_in(key, 201), shape, jnp.float32), -6.0, 6.0) * D ** (-0.5)
    second = jnp.clip(jax.random.normal(jax.random.fold_in(key, 202), shape, jnp.float32), -6.0, 6.0) * D ** (-0.5)
    return (first, second)


def draw_query_weight(key, part):
    first, second = head_weights(key)
    return first.astype(jnp.bfloat16)


def draw_key_weight(key, part):
    first, second = head_weights(key)
    return second.astype(jnp.bfloat16)


def block_scale(stream_key, dims, pieces, smallest, largest):
    loudness = 1.0
    for axis_at, parts in pieces:
        heights = jax.random.uniform(jax.random.fold_in(jax.random.fold_in(stream_key, 6), axis_at), (parts,), jnp.float32, smallest / len(pieces), largest / len(pieces))
        loudness = loudness * jnp.repeat(jnp.exp(heights), dims[axis_at] // parts).reshape((-1,) + (1,) * (len(dims) - 1 - axis_at))
    return loudness


def gaussian(rng, shape, spread, most, pieces=(), kind=jnp.bfloat16):
    values = jax.random.normal(rng, shape, jnp.float32) * spread
    if len(pieces) > 0:
        values = block_scale(rng, shape, pieces, -0.22, 0.18) * values
    return jnp.clip(values, min=-most, max=most).astype(kind)


def setup_inputs(seed: int = 0) -> dict:
    key_list = jax.random.split(jax.random.key(seed), 12)
    target = draw_target(jax.random.fold_in(key_list[11], 71), 0)
    source = draw_source(jax.random.fold_in(key_list[11], 71), 0)
    target_gains = jnp.clip(1.0 + 0.18 * jax.random.normal(key_list[2], (LAYERS, 4, D), jnp.float32), 0.099609375, 1.8984375).astype(jnp.bfloat16)
    source_gain = jnp.clip(1.0 + 0.18 * jax.random.normal(key_list[3], (LAYERS, D), jnp.float32), 0.099609375, 1.8984375).astype(jnp.bfloat16)
    query_weight = draw_query_weight(jax.random.fold_in(key_list[11], 71), 0)
    key_weight = draw_key_weight(jax.random.fold_in(key_list[11], 71), 0)
    value_weight = gaussian(key_list[6], (LAYERS, D, HEADS * HEAD_DIM), D ** -0.5, 0.1875, ((2, 2),))
    out_weight = gaussian(key_list[7], (LAYERS, HEADS * HEAD_DIM, D), (HEADS * HEAD_DIM) ** -0.5, 0.1875, ((1, 2),))
    gate_weight = gaussian(key_list[8], (LAYERS, D, FF), D ** -0.5, 0.1875, ((2, 2),))
    up_weight = gaussian(key_list[9], (LAYERS, D, FF), D ** -0.5, 0.1875, ((2, 2),))
    down_weight = gaussian(key_list[10], (LAYERS, FF, D), FF ** -0.5, 0.15625, ((1, 2),))
    return dict(target=target, source=source, target_gains=target_gains, source_gain=source_gain, query_weight=query_weight, key_weight=key_weight, value_weight=value_weight, out_weight=out_weight, gate_weight=gate_weight, up_weight=up_weight, down_weight=down_weight)


epsilon = 1e-06

def rms_norm(values, gain_row):
    widened = values.astype(jnp.float32)
    inverse = lax.rsqrt(lax.optimization_barrier(jnp.mean(widened * widened, axis=-1, keepdims=True)) + epsilon)
    return widened * inverse * gain_row.astype(jnp.float32)

def blockwise_sum(left, right, pieces_count):
    block_width = left.shape[1] // pieces_count
    summed = jnp.zeros((left.shape[0], right.shape[1]), jnp.float32)
    for index in range(pieces_count):
        partial_value = jnp.dot(left[:, index * block_width:(index + 1) * block_width], right[index * block_width:(index + 1) * block_width], preferred_element_type=jnp.float32)
        summed = summed + lax.optimization_barrier(partial_value.astype(jnp.bfloat16)).astype(jnp.float32)
    return summed.astype(jnp.bfloat16)

def reference(target, source, target_gains, source_gain, query_weight, key_weight, value_weight, out_weight, gate_weight, up_weight, down_weight):
    factor = HEAD_DIM ** (-0.5)
    stream = target
    for layer_index in range(LAYERS):
        layer_gains = target_gains[layer_index]
        normed_source = rms_norm(source, source_gain[layer_index]).astype(jnp.bfloat16)
        key_rows = jnp.dot(normed_source, key_weight[layer_index], preferred_element_type=jnp.float32).astype(jnp.bfloat16)
        value_rows = jnp.dot(normed_source, value_weight[layer_index], preferred_element_type=jnp.float32).astype(jnp.bfloat16)
        key_wide = key_rows.astype(jnp.float32).reshape(SRC, HEADS, HEAD_DIM)
        value_wide = value_rows.astype(jnp.float32).reshape(SRC, HEADS, HEAD_DIM)
        normed = rms_norm(stream, layer_gains[0]).astype(jnp.bfloat16)
        queries = jnp.dot(normed, query_weight[layer_index], preferred_element_type=jnp.float32).astype(jnp.bfloat16)
        query_blocks = queries.astype(jnp.float32).reshape(TGT // TGT_DEV, TGT_DEV, HEADS, HEAD_DIM)

        def attend(query_block):
            scores = jnp.einsum('thd,shd->ths', query_block, key_wide) * factor
            row_max = lax.optimization_barrier(jnp.max(scores, axis=-1, keepdims=True))
            weights = jnp.exp(scores - row_max)
            totals = lax.optimization_barrier(jnp.sum(weights, axis=-1))
            rounded = lax.optimization_barrier(weights.astype(jnp.bfloat16)).astype(jnp.float32)
            blended = jnp.einsum('ths,shd->thd', rounded, value_wide)
            return (blended / totals[..., None]).astype(jnp.bfloat16)
        context = lax.map(attend, query_blocks).reshape(TGT, HEADS * HEAD_DIM)
        attended = blockwise_sum(context, out_weight[layer_index], N_TP)
        stream = (stream.astype(jnp.float32) + rms_norm(attended, layer_gains[1])).astype(jnp.bfloat16)
        mixer_in = rms_norm(stream, layer_gains[2]).astype(jnp.bfloat16)
        gate_part = jnp.dot(mixer_in, gate_weight[layer_index], preferred_element_type=jnp.float32)
        up_part = jnp.dot(mixer_in, up_weight[layer_index], preferred_element_type=jnp.float32)
        hidden = (jax.nn.silu(gate_part) * up_part).astype(jnp.bfloat16)
        mixer_out = blockwise_sum(hidden, down_weight[layer_index], N_TP)
        stream = (stream.astype(jnp.float32) + rms_norm(mixer_out, layer_gains[3])).astype(jnp.bfloat16)
    return stream
```

```python
import functools

import jax
import jax.numpy as jnp
from jax import lax
from jax.experimental import pallas as pl
from jax.experimental.pallas import tpu as pltpu
from jax.sharding import PartitionSpec as P

HEAD_DIM = 128
AXES = ("sp", "tp")
epsilon = 1e-06


def scaled(values):
    return values * lax.rsqrt(jnp.mean(values * values, axis=-1, keepdims=True) + epsilon)


def dot(left, right, left_dim=1, right_dim=0):
    return lax.dot_general(
        left,
        right,
        (((left_dim,), (right_dim,)), ((), ())),
        preferred_element_type=jnp.float32,
    )


def rolled(ref, blocks, block_rows):
    if blocks == 0:
        return ref[...].astype(jnp.float32)
    cut = ref.shape[0] - blocks * block_rows
    return jnp.concatenate([ref[cut:, :], ref[:cut, :]], axis=0).astype(jnp.float32)


def updated_stream(stream, parts, gain, own_rows):
    total = rolled(parts[0], 0, own_rows)
    for shift in range(1, len(parts)):
        total = total + rolled(parts[shift], shift, own_rows)
    total = total.astype(jnp.bfloat16).astype(jnp.float32)
    return (stream.astype(jnp.float32) + scaled(total) * gain).astype(jnp.bfloat16)


def source_kernel(layers, pieces, *refs):
    rows = refs[:pieces]
    gain, key_weight, value_weight = refs[pieces : pieces + 3]
    keys, values = refs[pieces + 3 :]
    at = 0
    for piece in rows:
        count = piece.shape[0]
        normed = scaled(piece[...].astype(jnp.float32))
        for layer in range(layers):
            mixed = (normed * gain[layer : layer + 1, :].astype(jnp.float32)).astype(jnp.bfloat16)
            keys[layer, at : at + count, :] = dot(mixed, key_weight[layer]).astype(jnp.bfloat16)
            values[layer, at : at + count, :] = dot(mixed, value_weight[layer]).astype(jnp.bfloat16)
        at += count


def attention_kernel(layer, own_rows, streams, parts, chunks, *refs):
    refs = list(refs)
    stream_refs = [refs.pop(0) for _ in range(streams)]
    part_refs = [refs.pop(0) for _ in range(parts)]
    key_refs = [refs.pop(0) for _ in range(chunks)]
    value_refs = [refs.pop(0) for _ in range(chunks)]
    gains, query_weight, out_weight = refs[:3]
    if parts:
        stream_out, partial_out = refs[3:5]
    else:
        (partial_out,) = refs[3:4]
    gain = gains[...].astype(jnp.float32)
    stream = jnp.concatenate([ref[...] for ref in stream_refs], axis=0)
    if parts:
        stream = updated_stream(stream, part_refs, gain[4 * layer - 1 : 4 * layer, :], own_rows)
        stream_out[...] = stream
    normed = (scaled(stream.astype(jnp.float32)) * gain[4 * layer : 4 * layer + 1, :]).astype(
        jnp.bfloat16
    )
    queries = dot(normed, query_weight[0]).astype(jnp.bfloat16)
    factor = HEAD_DIM ** (-0.5)
    contexts = []
    for head in range(queries.shape[1] // HEAD_DIM):
        columns = slice(head * HEAD_DIM, (head + 1) * HEAD_DIM)
        query = queries[:, columns]
        scores = [dot(ref[0, :, columns], query, 1, 1) * factor for ref in key_refs]
        largest = functools.reduce(
            jnp.maximum, [jnp.max(block, axis=0, keepdims=True) for block in scores]
        )
        total = 0.0
        weighted = 0.0
        for block, ref in zip(scores, value_refs):
            weights = jnp.exp(block - largest)
            total = total + jnp.sum(weights, axis=0, keepdims=True)
            weighted = weighted + dot(ref[0, :, columns], weights.astype(jnp.bfloat16), 0, 0)
        contexts.append((weighted / total).astype(jnp.bfloat16))
    context = jnp.concatenate(contexts, axis=0)
    partial_out[...] = dot(context, out_weight[0], 0, 0).astype(jnp.bfloat16)


def mixer_kernel(layer, own_rows, streams, parts, *refs):
    refs = list(refs)
    stream_refs = [refs.pop(0) for _ in range(streams)]
    part_refs = [refs.pop(0) for _ in range(parts)]
    gains, gate_weight, up_weight, down_weight, stream_out, partial_out = refs
    gain = gains[...].astype(jnp.float32)
    stream = jnp.concatenate([ref[...] for ref in stream_refs], axis=0)
    at = 4 * layer
    stream = updated_stream(stream, part_refs, gain[at + 1 : at + 2, :], own_rows)
    stream_out[...] = stream
    mixed = (scaled(stream.astype(jnp.float32)) * gain[at + 2 : at + 3, :]).astype(jnp.bfloat16)
    gate = dot(mixed, gate_weight[0])
    up = dot(mixed, up_weight[0])
    hidden = (gate / (1.0 + jnp.exp(-gate)) * up).astype(jnp.bfloat16)
    partial_out[...] = dot(hidden, down_weight[0]).astype(jnp.bfloat16)


def final_kernel(layers, own_rows, parts, *refs):
    stream = refs[0][...]
    gains, out = refs[1 + parts :]
    gain = gains[...].astype(jnp.float32)[4 * layers - 1 : 4 * layers, :]
    total = refs[1][...].astype(jnp.float32)
    for ref in refs[2 : 1 + parts]:
        total = total + ref[...].astype(jnp.float32)
    total = total.astype(jnp.bfloat16).astype(jnp.float32)
    out[...] = (stream.astype(jnp.float32) + scaled(total) * gain).astype(jnp.bfloat16)


def whole(array):
    return pl.BlockSpec(array.shape, lambda i: (0,) * array.ndim)


def one_layer(array, layer):
    return pl.BlockSpec((1,) + array.shape[1:], lambda i: (layer,) + (0,) * (array.ndim - 1))


def call(kernel, specs_and_arrays, outs, flops, name, vmem=None):
    specs = [entry[0] for entry in specs_and_arrays]
    arrays = [entry[1] for entry in specs_and_arrays]
    return pl.pallas_call(
        kernel,
        grid=(1,),
        in_specs=specs,
        out_specs=[whole(out) for out in outs],
        out_shape=outs,
        name=name,
        cost_estimate=pl.CostEstimate(flops=flops, transcendentals=0, bytes_accessed=0),
        compiler_params=pltpu.CompilerParams(vmem_limit_bytes=vmem),
    )(*arrays)


def per_device(
    target,
    source,
    target_gains,
    source_gain,
    query_weight,
    key_weight,
    value_weight,
    out_weight,
    gate_weight,
    up_weight,
    down_weight,
):
    layers, width, columns = query_weight.shape
    units = gate_weight.shape[2]
    own_rows = target.shape[0]
    sp_count = lax.axis_size("sp")
    tp_count = lax.axis_size("tp")
    group_rows = own_rows * tp_count
    bf16 = jnp.bfloat16

    def permuted(array, place):
        pairs = []
        for sp_at in range(sp_count):
            for tp_at in range(tp_count):
                to_sp, to_tp = place(sp_at, tp_at)
                pairs.append((sp_at * tp_count + tp_at, to_sp * tp_count + to_tp))
        return lax.ppermute(array, AXES, pairs)

    def around_tp(array):
        return [array] + [
            permuted(array, lambda s, t, shift=shift: (s, (t - shift) % tp_count))
            for shift in range(1, tp_count)
        ]

    piece_rows = source.shape[0] // tp_count
    piece = lax.dynamic_slice_in_dim(source, lax.axis_index("tp") * piece_rows, piece_rows, 0)
    planes = sp_count // 4
    groups = [piece] + [
        permuted(piece, lambda s, t, shift=shift: ((s + 4 * shift) % sp_count, t))
        for shift in range(1, planes)
    ]
    chunks = []
    for group in groups:
        for step in range(2):
            other = permuted(group, lambda s, t, step=step: (s ^ (1 + (t + step) % 2), t))
            group = jnp.concatenate([group, other], axis=0)
        chunks.append(around_tp(group))

    streams = around_tp(target)

    keys = []
    values = []
    for chunk in chunks:
        rows = sum(entry.shape[0] for entry in chunk)
        out = jax.ShapeDtypeStruct((layers, rows, columns), bf16)
        made = call(
            functools.partial(source_kernel, layers, len(chunk)),
            [(whole(entry), entry) for entry in chunk]
            + [(whole(entry), entry) for entry in (source_gain, key_weight, value_weight)],
            [out, out],
            4 * layers * rows * width * columns,
            "source_rows",
            32 * 2**20,
        )
        keys.append(made[0])
        values.append(made[1])

    gains = target_gains.reshape(layers * 4, width)
    square = jax.ShapeDtypeStruct((group_rows, width), bf16)
    parts = []
    for layer in range(layers):
        arrays = [(whole(entry), entry) for entry in streams + parts]
        arrays += [(one_layer(entry, layer), entry) for entry in keys + values]
        arrays += [(whole(gains), gains)]
        arrays += [(one_layer(entry, layer), entry) for entry in (query_weight, out_weight)]
        made = call(
            functools.partial(
                attention_kernel, layer, own_rows, len(streams), len(parts), len(keys)
            ),
            arrays,
            [square, square] if parts else [square],
            4 * group_rows * columns * (width + 2 * sp_count * source.shape[0]),
            "attention",
            40 * 2**20,
        )
        if parts:
            streams = [made[0]]
        parts = around_tp(made[-1])
        arrays = [(whole(entry), entry) for entry in streams + parts]
        arrays += [(whole(gains), gains)]
        arrays += [
            (one_layer(entry, layer), entry) for entry in (gate_weight, up_weight, down_weight)
        ]
        made = call(
            functools.partial(mixer_kernel, layer, own_rows, len(streams), len(parts)),
            arrays,
            [square, square],
            6 * group_rows * width * units,
            "mixer",
            40 * 2**20,
        )
        streams = [made[0]]
        if layer + 1 < layers:
            parts = around_tp(made[1])
    mine = jax.ShapeDtypeStruct((own_rows, width), bf16)
    partial = made[1]
    parts = [partial[:own_rows]]
    for shift in range(1, tp_count):
        away = (tp_count - shift) * own_rows
        parts.append(
            permuted(
                partial[away : away + own_rows],
                lambda s, t, shift=shift: (s, (t - shift) % tp_count),
            )
        )
    last = streams[0][:own_rows]
    return call(
        functools.partial(final_kernel, layers, own_rows, len(parts)),
        [(whole(entry), entry) for entry in [last] + parts + [gains]],
        [mine],
        0,
        "last_stream",
        8 * 2**20,
    )[0]


def solution(mesh):
    placed = (
        P(("sp", "tp"), None),
        P("sp", None),
        P(),
        P(),
        P(None, None, "tp"),
        P(None, None, "tp"),
        P(None, None, "tp"),
        P(None, "tp", None),
        P(None, None, "tp"),
        P(None, None, "tp"),
        P(None, "tp", None),
    )
    return jax.shard_map(
        per_device, mesh=mesh, in_specs=placed, out_specs=P(("sp", "tp"), None), check_vma=False
    )
```
